32 devices in a mesh: rep: 2 (over y), fs: 4 (over z), tp: 4 (over x, core).
Axes of the slice: x: 2, y: 2, z: 4, core: 2. Of those that a mesh axis runs over, the one named last changes fastest.
Arguments:
- tokens: bfloat16 [2048, 2048], P(('rep', 'fs')), may hold values from -6 to 6
- mix_gain: float32 [2048], replicated, may hold values from 0.1 to 1.9
- group_weight: float32 [512, 2048], P('fs', 'tp'), may hold values from -0.25 to 0.25
- group_scale: float32 [1, 2048], P(None, 'tp'), may hold values from 0.5 to 2
- mlp_gain: float32 [2048], replicated, may hold values from 0.1 to 1.9
- up_weight: float32 [2048, 8192], P('fs', 'tp'), may hold values from -0.125 to 0.125
- up_scale: float32 [1, 8192], P(None, 'tp'), may hold values from 0.5 to 2
- down_weight: float32 [8192, 2048], P('tp', 'fs'), may hold values from -0.0625 to 0.0625
- down_scale: float32 [1, 2048], replicated, may hold values from 0.5 to 2
Outputs:
- layer_out: bfloat16 [2048, 2048], P(('rep', 'fs'))
The draws below stay inside these ranges and needn't reach their ends.
All inputs are finite; a program needn't handle non-finite values.
Results may differ from the reference program's by a relative error of at most 0.013.
Values may be sent and summed in bfloat16 or wider, within the bound.
No kernel may reach another device: no remote copies, remote signals or barrier semaphores. Data moves between devices by JAX's collectives and lax.ppermute only.
A program may use at most 64 MiB of HBM per device.

```python
import math
import jax
import jax.numpy as jnp
from jax import lax

D = 2048
FF = 8192
GROUPS = 4
GROUP_DIM = 512
LENGTH = 128
TOKENS = 2048
N_TP = 4


def shard_levels(stream_key, dims, cuts, smallest, high):
    level, own = 1.0, jax.random.fold_in(stream_key, 6)
    for dim, blocks in cuts:
        steps = jnp.exp(jax.random.uniform(jax.random.fold_in(own, dim), (blocks,), jnp.float32, smallest / len(cuts), high / len(cuts)))
        level = level * jnp.repeat(steps, dims[dim] // blocks).reshape([-1 if axis == dim else 1 for axis in range(len(dims))])
    return level


def gaussian(rng, shape, spread, most, shards=(), kind=jnp.bfloat16):
    values = jax.random.normal(rng, shape, jnp.float32) * spread
    if len(shards) > 0:
        values = shard_levels(rng, shape, shards, -0.22, 0.18) * values
    return jnp.clip(values, min=-most, max=most).astype(kind)


def setup_inputs(seed: int = 0) -> dict:
    keys = jax.random.split(jax.random.key(seed), 10)
    tokens = gaussian(keys[0], (TOKENS, D), 1.0, 6.0, ((0, 8),))
    mix_gain = jnp.clip(1.0 + 0.18 * jax.random.normal(keys[1], (D,), jnp.float32), 0.1, 1.9)
    group_weight = gaussian(keys[2], (GROUP_DIM, D), GROUP_DIM ** -0.5, 0.25, ((0, 4), (1, 4)), jnp.float32)
    group_scale = jnp.clip(jnp.exp(math.log(2.0) - 1.3862944 * jax.random.uniform(keys[3], (1, D), jnp.float32) ** shard_levels(keys[3], (1, D), ((1, 4),), -0.2, 0.2)), 0.5, 2.0)
    mlp_gain = jnp.clip(1.0 + 0.18 * jax.random.normal(keys[4], (D,), jnp.float32), 0.1, 1.9)
    up_weight = gaussian(keys[5], (D, FF), D ** -0.5, 0.125, ((0, 4), (1, 4)), jnp.float32)
    up_scale = jnp.clip(jnp.exp(math.log(2.0) - 1.3862944 * jax.random.uniform(keys[6], (1, FF), jnp.float32) ** shard_levels(keys[6], (1, FF), ((1, 4),), -0.2, 0.2)), 0.5, 2.0)
    down_weight = gaussian(keys[7], (FF, D), FF ** -0.5, 0.0625, ((0, 4), (1, 4)), jnp.float32)
    down_scale = jnp.clip(jnp.exp(jax.random.uniform(keys[8], (1, D), jnp.float32, math.log(0.5), math.log(2.0))), 0.5, 2.0)
    return {"tokens": tokens, "mix_gain": mix_gain, "group_weight": group_weight, "group_scale": group_scale, "mlp_gain": mlp_gain, "up_weight": up_weight, "up_scale": up_scale, "down_weight": down_weight, "down_scale": down_scale}


norm_eps = 1e-06

def norm_rows(values, gain):
    promoted = values.astype(jnp.float32)
    inverse = lax.rsqrt(lax.optimization_barrier(jnp.mean(promoted * promoted, axis=-1, keepdims=True)) + norm_eps)
    return (promoted * inverse * gain.astype(jnp.float32)).astype(jnp.bfloat16)

def band_means(inputs, window, seq_length):
    row_count, columns = inputs.shape
    by_sequence = inputs.reshape(row_count // seq_length, seq_length, columns)
    position = jnp.arange(seq_length, dtype=jnp.int32)
    offset = position[:, None] - position[None, :]
    band_mask = ((offset >= 0) & (offset < window)).astype(jnp.float32)
    divisor = jnp.minimum(position + 1, window).astype(jnp.float32)
    summed = jnp.einsum('ts,nsc->ntc', band_mask, by_sequence, precision=lax.Precision.HIGHEST)
    return (summed / divisor[None, :, None] - by_sequence).reshape(row_count, columns)

def reference(tokens, mix_gain, group_weight, group_scale, mlp_gain, up_weight, up_scale, down_weight, down_scale):
    normed = norm_rows(tokens, mix_gain).astype(jnp.float32)
    pieces = []
    for group_index in range(GROUPS):
        first_col = group_index * GROUP_DIM
        inputs = normed[:, first_col:first_col + GROUP_DIM]
        pooled = band_means(inputs, 2 ** (group_index + 1), LENGTH).astype(jnp.bfloat16)
        weight_cols = group_weight[:, first_col:first_col + GROUP_DIM].astype(jnp.bfloat16)
        product = jnp.dot(pooled, weight_cols, preferred_element_type=jnp.float32)
        pieces.append(product * group_scale[:, first_col:first_col + GROUP_DIM])
    mixed_cols = jnp.concatenate(pieces, axis=1)
    carried = (tokens.astype(jnp.float32) + mixed_cols).astype(jnp.bfloat16)
    normed_mlp = norm_rows(carried, mlp_gain)
    pre_act = jnp.dot(normed_mlp, up_weight.astype(jnp.bfloat16), preferred_element_type=jnp.float32) * up_scale
    hidden = jnp.square(jax.nn.relu(pre_act)).astype(jnp.bfloat16)
    tp_block = FF // N_TP
    summed = jnp.zeros(carried.shape, jnp.float32)
    for tp_index in range(N_TP):
        rows_here = slice(tp_index * tp_block, (tp_index + 1) * tp_block)
        partial_value = jnp.dot(hidden[:, rows_here], down_weight[rows_here].astype(jnp.bfloat16), preferred_element_type=jnp.float32) * down_scale
        summed = summed + partial_value.astype(jnp.bfloat16).astype(jnp.float32)
    return (carried.astype(jnp.float32) + summed).astype(jnp.bfloat16)
```

```python
import jax
import jax.numpy as jnp
from jax import lax
from jax.sharding import PartitionSpec as P

GROUPS = 4
LENGTH = 128


norm_eps = 1e-06


def norm_rows(values, gain):
    promoted = values.astype(jnp.float32)
    inverse = lax.rsqrt(jnp.mean(promoted * promoted, axis=-1, keepdims=True) + norm_eps)
    return (promoted * inverse * gain).astype(jnp.bfloat16)


def band_means(inputs, window, seq_length):
    row_count, columns = inputs.shape
    by_sequence = inputs.reshape(row_count // seq_length, seq_length, columns)
    position = jnp.arange(seq_length, dtype=jnp.int32)
    offset = position[:, None] - position[None, :]
    band_mask = ((offset >= 0) & (offset < window)).astype(jnp.bfloat16)
    divisor = jnp.minimum(position + 1, window).astype(jnp.float32)
    summed = jnp.einsum("ts,nsc->ntc", band_mask, by_sequence, preferred_element_type=jnp.float32)
    return (summed / divisor[None, :, None] - by_sequence.astype(jnp.float32)).reshape(
        row_count, columns
    )


def gather_body(
    tokens,
    mix_gain,
    group_weight,
    group_scale,
    mlp_gain,
    up_weight,
    up_scale,
    down_weight,
    down_scale,
):
    model_width = tokens.shape[1]
    group_width = model_width // GROUPS
    own_cols = group_weight.shape[1]
    column_start = lax.axis_index("tp") * own_cols
    group_index = column_start // group_width
    normed = norm_rows(tokens, mix_gain)
    inputs = lax.dynamic_slice_in_dim(normed, group_index * group_width, group_width, 1)
    window = jnp.left_shift(jnp.int32(2), group_index)
    pooled = band_means(inputs, window, LENGTH).astype(jnp.bfloat16)
    mixed_cols = (
        jnp.dot(
            pooled,
            lax.all_gather(group_weight.astype(jnp.bfloat16), "fs", axis=0, tiled=True),
            preferred_element_type=jnp.float32,
        )
        * group_scale
    )
    own_tokens = lax.dynamic_slice_in_dim(tokens, column_start, own_cols, 1)
    carried_cols = (own_tokens.astype(jnp.float32) + mixed_cols).astype(jnp.bfloat16)
    carried = lax.all_gather(carried_cols, "tp", axis=1, tiled=True)
    normed_mlp = norm_rows(carried, mlp_gain)
    pre_act = (
        jnp.dot(
            normed_mlp,
            lax.all_gather(up_weight.astype(jnp.bfloat16), "fs", axis=0, tiled=True),
            preferred_element_type=jnp.float32,
        )
        * up_scale
    )
    hidden = jnp.square(jax.nn.relu(pre_act)).astype(jnp.bfloat16)
    partial_value = (
        jnp.dot(
            hidden,
            lax.all_gather(down_weight.astype(jnp.bfloat16), "fs", axis=1, tiled=True),
            preferred_element_type=jnp.float32,
        )
        * down_scale
    )
    summed = lax.psum(partial_value.astype(jnp.bfloat16), "tp").astype(jnp.float32)
    return (carried.astype(jnp.float32) + summed).astype(jnp.bfloat16)


def bits_of(count):
    return [1 << b for b in range(count.bit_length() - 1)]


def exchange_body(sizes):
    reps, n, m = sizes["rep"], sizes["fs"], sizes["tp"]
    axes = ("rep", "fs", "tp")

    def hop(values, rep=0, fs=0, tp=0):
        pairs = []
        for a in range(reps):
            for b in range(n):
                for c in range(m):
                    target = (((a + rep) % reps) * n + (b ^ fs)) * m + (c ^ tp)
                    pairs.append(((a * n + b) * m + c, target))
        return lax.ppermute(values, axes, pairs)

    def pick(stacked, index, axis=0):
        return lax.dynamic_index_in_dim(stacked, index, axis, keepdims=False)

    def reorder(stacked, mask):
        return jnp.stack([pick(stacked, k ^ mask) for k in range(stacked.shape[0])])

    def spread_fs(own):
        held = [own]
        for d in range(1, n):
            low = d & -d
            held.append(hop(held[d ^ low], fs=low))
        return held

    def gather_tp(own):
        held = own[None]
        order = [0]
        for bit in reversed(bits_of(m)):
            held = jnp.concatenate([held, hop(held, tp=bit)])
            order += [e ^ bit for e in order]
        places = [order.index(e) for e in range(m)]
        return jnp.stack([held[p] for p in places])

    def swap_weights(send):
        r = lax.axis_index("rep")
        got = []
        for d in range(n):
            block = send(d)
            if d == 0:
                got.append(block.astype(jnp.bfloat16))
                continue
            rows = block.shape[0] // reps
            part = lax.dynamic_slice_in_dim(block, r * rows, rows, 0).astype(jnp.bfloat16)
            part = hop(part, fs=d)
            parts = [part] + [hop(part, rep=k) for k in range(1, reps)]
            stacked = jnp.stack(parts)
            got.append(
                jnp.concatenate([pick(stacked, lax.rem(r - k + reps, reps)) for k in range(reps)])
            )
        return got

    def body(
        tokens,
        mix_gain,
        group_weight,
        group_scale,
        mlp_gain,
        up_weight,
        up_scale,
        down_weight,
        down_scale,
    ):
        rows, model_width = tokens.shape
        i, j = lax.axis_index("fs"), lax.axis_index("tp")
        width = group_weight.shape[1]
        units = up_weight.shape[1] // n
        cols = down_weight.shape[1]
        start = j * width

        promoted = tokens.astype(jnp.float32)
        inverse = lax.rsqrt(jnp.mean(promoted * promoted, axis=-1, keepdims=True) + norm_eps)
        own_tokens = lax.dynamic_slice_in_dim(tokens, start, width, 1)
        all_tokens = spread_fs(own_tokens)
        all_inverse = spread_fs(inverse.reshape(1, rows))
        mixer = spread_fs(group_weight.astype(jnp.bfloat16))
        mixer = reorder(jnp.stack(mixer), i).reshape(-1, width)

        ups = swap_weights(
            lambda d: lax.dynamic_slice_in_dim(up_weight, (i ^ d) * units, units, 1)
        )
        downs = swap_weights(
            lambda d: lax.dynamic_slice_in_dim(down_weight, (i ^ d) * units, units, 0)
        )

        gain = lax.dynamic_slice_in_dim(mix_gain, start, width, 0)
        window = jnp.left_shift(jnp.int32(2), j)
        blocks = []
        for d in range(n):
            block = all_tokens[d].astype(jnp.float32)
            normed = (block * all_inverse[d].reshape(rows, 1) * gain).astype(jnp.bfloat16)
            pooled = band_means(normed, window, LENGTH).astype(jnp.bfloat16)
            mixed = jnp.dot(pooled, mixer, preferred_element_type=jnp.float32) * group_scale
            carried_cols = (block + mixed).astype(jnp.bfloat16)
            blocks.append(reorder(gather_tp(carried_cols), i ^ j))
        carried = jnp.stack(blocks)
        sq = carried.astype(jnp.float32)
        mean = jnp.sum(sq * sq, axis=(1, 3), keepdims=True) / model_width
        mlp_gains = reorder(mlp_gain.reshape(n, 1, cols), i)
        normed_mlp = (sq * lax.rsqrt(mean + norm_eps) * mlp_gains).astype(jnp.bfloat16)
        pre_act = jnp.einsum(
            "acrw,cwu->aru", normed_mlp, jnp.stack(ups), preferred_element_type=jnp.float32
        ) * lax.dynamic_slice_in_dim(up_scale, i * units, units, 1)
        hidden = jnp.square(jax.nn.relu(pre_act)).astype(jnp.bfloat16)

        sums = []
        for d in range(n):
            scale = lax.dynamic_slice_in_dim(down_scale, (i ^ d) * cols, cols, 1)
            part = jnp.einsum(
                "aru,uc->arc", hidden, downs[d], preferred_element_type=jnp.float32
            ) * scale
            part = part.astype(jnp.bfloat16)
            for bit in bits_of(m):
                split = part.reshape(n, 2, part.shape[1] // 2, cols)
                mine = (j // bit) % 2
                keep = pick(split, mine, 1)
                got = hop(pick(split, 1 - mine, 1), tp=bit)
                part = (keep.astype(jnp.float32) + got.astype(jnp.float32)).astype(jnp.bfloat16)
            sums.append(part)
        sums = jnp.stack(sums, 1)
        total = sums[0].astype(jnp.float32)
        for e in range(1, n):
            got = hop(sums[e], fs=e).astype(jnp.float32)
            total = total + jnp.stack([got[c ^ e] for c in range(n)])
        own = carried[0]
        for bit in bits_of(m):
            split = own.reshape(n, 2, own.shape[1] // 2, cols)
            own = pick(split, (j // bit) % 2, 1)
        out = (own.astype(jnp.float32) + total).astype(jnp.bfloat16)
        out = reorder(gather_tp(out), j)
        shape = [2] * len(bits_of(m)) + [n, out.shape[2], cols]
        out = out.reshape(shape)
        k = len(bits_of(m))
        out = out.transpose(tuple(reversed(range(k))) + (k, k + 1, k + 2))
        out = out.reshape(m, n, -1, cols).transpose(0, 2, 1, 3).reshape(rows, n, cols)
        out = jnp.stack([pick(out, c ^ i, 1) for c in range(n)], 1)
        return out.reshape(rows, model_width)

    return body


def solution(mesh):
    in_specs = (
        P(("rep", "fs"), None),
        P(),
        P("fs", "tp"),
        P(None, "tp"),
        P(),
        P("fs", "tp"),
        P(None, "tp"),
        P("tp", "fs"),
        P(),
    )
    out_specs = P(("rep", "fs"), None)
    sizes = dict(mesh.shape)

    def layer(*args):
        tokens, mixer, up = args[0], args[2], args[5]
        moved = up.size // sizes["tp"]
        gathered = tokens.size // sizes["rep"]
        powers = all(sizes[a] & (sizes[a] - 1) == 0 for a in ("fs", "tp"))
        fits = sizes["tp"] == sizes["fs"] == GROUPS
        chosen = exchange_body(sizes) if powers and fits and gathered < moved else gather_body
        return jax.shard_map(
            chosen, mesh=mesh, in_specs=in_specs, out_specs=out_specs, check_vma=False
        )(*args)

    return layer
```

```python
import functools
import math

import jax
import jax.numpy as jnp
from jax import lax
from jax.experimental import pallas as pl
from jax.experimental.pallas import tpu as pltpu
from jax.sharding import PartitionSpec as P


GROUPS = 4
LENGTH = 128


norm_eps = 1e-06


def norm_rows(values, gain):
    promoted = values.astype(jnp.float32)
    inverse = lax.rsqrt(jnp.mean(promoted * promoted, axis=-1, keepdims=True) + norm_eps)
    return (promoted * inverse * gain).astype(jnp.bfloat16)


def band_means(inputs, window, seq_length):
    row_count, columns = inputs.shape
    by_sequence = inputs.reshape(row_count // seq_length, seq_length, columns)
    position = jnp.arange(seq_length, dtype=jnp.int32)
    offset = position[:, None] - position[None, :]
    band_mask = ((offset >= 0) & (offset < window)).astype(jnp.bfloat16)
    divisor = jnp.minimum(position + 1, window).astype(jnp.float32)
    summed = jnp.einsum("ts,nsc->ntc", band_mask, by_sequence, preferred_element_type=jnp.float32)
    return (summed / divisor[None, :, None] - by_sequence.astype(jnp.float32)).reshape(
        row_count, columns
    )


def gather_body(
    tokens,
    mix_gain,
    group_weight,
    group_scale,
    mlp_gain,
    up_weight,
    up_scale,
    down_weight,
    down_scale,
):
    model_width = tokens.shape[1]
    group_width = model_width // GROUPS
    own_cols = group_weight.shape[1]
    column_start = lax.axis_index("tp") * own_cols
    group_index = column_start // group_width
    normed = norm_rows(tokens, mix_gain)
    inputs = lax.dynamic_slice_in_dim(normed, group_index * group_width, group_width, 1)
    window = jnp.left_shift(jnp.int32(2), group_index)
    pooled = band_means(inputs, window, LENGTH).astype(jnp.bfloat16)
    mixed_cols = (
        jnp.dot(
            pooled,
            lax.all_gather(group_weight.astype(jnp.bfloat16), "fs", axis=0, tiled=True),
            preferred_element_type=jnp.float32,
        )
        * group_scale
    )
    own_tokens = lax.dynamic_slice_in_dim(tokens, column_start, own_cols, 1)
    carried_cols = (own_tokens.astype(jnp.float32) + mixed_cols).astype(jnp.bfloat16)
    carried = lax.all_gather(carried_cols, "tp", axis=1, tiled=True)
    normed_mlp = norm_rows(carried, mlp_gain)
    pre_act = (
        jnp.dot(
            normed_mlp,
            lax.all_gather(up_weight.astype(jnp.bfloat16), "fs", axis=0, tiled=True),
            preferred_element_type=jnp.float32,
        )
        * up_scale
    )
    hidden = jnp.square(jax.nn.relu(pre_act)).astype(jnp.bfloat16)
    partial_value = (
        jnp.dot(
            hidden,
            lax.all_gather(down_weight.astype(jnp.bfloat16), "fs", axis=1, tiled=True),
            preferred_element_type=jnp.float32,
        )
        * down_scale
    )
    summed = lax.psum(partial_value.astype(jnp.bfloat16), "tp").astype(jnp.float32)
    return (carried.astype(jnp.float32) + summed).astype(jnp.bfloat16)


def bits_of(count):
    return [1 << b for b in range(count.bit_length() - 1)]


def local(kernel, outs, scalars, *arrays, scratch=(), flops=0):
    moved = sum(a.size * a.dtype.itemsize for a in (*arrays, *outs))
    held = moved + sum(math.prod(shape) * jnp.dtype(kind).itemsize for shape, kind in scratch)
    return pl.pallas_call(
        kernel,
        out_shape=outs,
        in_specs=[pl.BlockSpec(memory_space=pltpu.SMEM)]
        + [pl.BlockSpec(memory_space=pltpu.VMEM)] * len(arrays),
        out_specs=[pl.BlockSpec(memory_space=pltpu.VMEM)] * len(outs),
        scratch_shapes=[pltpu.VMEM(shape, kind) for shape, kind in scratch],
        compiler_params=pltpu.CompilerParams(vmem_limit_bytes=min(3 * held + (8 << 20), 60 << 20)),
        cost_estimate=pl.CostEstimate(flops=max(flops, 1 << 20), bytes_accessed=moved, transcendentals=0),
    )(jnp.stack([jnp.int32(v) for v in scalars]), *arrays)


def array(shape, kind=jnp.bfloat16):
    return jax.ShapeDtypeStruct(shape, kind)


def at(index, size):
    return pl.ds(pl.multiple_of(index * size, size), size)


def prep_kernel(scalars, tokens, packed):
    rows, width = tokens.shape[0], packed.shape[1]
    promoted = tokens[...].astype(jnp.float32)
    inverse = lax.rsqrt(jnp.mean(promoted * promoted, axis=-1, keepdims=True) + norm_eps)
    lane = lax.broadcasted_iota(jnp.int32, (rows, 128), 1)
    pieces = jnp.zeros((rows, 128), jnp.float32)
    for place in range(3):
        piece = inverse.astype(jnp.bfloat16).astype(jnp.float32)
        pieces = jnp.where(lane == place, piece, pieces)
        inverse = inverse - piece
    packed[:rows, :] = tokens[:, at(scalars[0], width)]
    packed[rows:, :] = jnp.zeros((packed.shape[0] - rows, width), jnp.bfloat16)
    packed[rows:, :rows] = jnp.transpose(pieces)[: packed.shape[0] - rows].astype(jnp.bfloat16)


def mix_kernel(scalars, packed, gain, scale, *refs):
    *pieces, carried, mixer = refs
    rows, depth = carried.shape[0], pieces[0].shape[0]
    for d, piece in enumerate(pieces):
        mixer[at(scalars[0] ^ d, depth), :] = piece[...]
    tokens = packed[:rows, :].astype(jnp.float32)
    three = packed[rows:, :rows].astype(jnp.float32)
    inverse = three[0:1] + three[1:2] + three[2:3]
    inverse = jnp.transpose(jnp.broadcast_to(inverse, (128, rows)))[:, :1]
    normed = (tokens * inverse * gain[...]).astype(jnp.bfloat16)
    window = jnp.left_shift(jnp.int32(2), scalars[1])
    row = lax.broadcasted_iota(jnp.int32, (LENGTH, LENGTH), 0)
    offset = row - lax.broadcasted_iota(jnp.int32, (LENGTH, LENGTH), 1)
    band = jnp.where((offset >= 0) & (offset < window), 1.0, 0.0).astype(jnp.bfloat16)
    position = lax.broadcasted_iota(jnp.int32, (LENGTH, 1), 0)
    divisor = jnp.minimum(position + 1, window).astype(jnp.float32)
    for first in range(0, rows, LENGTH):
        here = slice(first, first + LENGTH)
        summed = jnp.dot(band, normed[here], preferred_element_type=jnp.float32)
        pooled = (summed / divisor - normed[here].astype(jnp.float32)).astype(jnp.bfloat16)
        mixed = jnp.dot(pooled, mixer[...], preferred_element_type=jnp.float32) * scale[...]
        carried[here, :] = (tokens[here] + mixed).astype(jnp.bfloat16)


def norm_kernel(scalars, gain, *refs):
    *columns, normed, kept = refs
    rows, width = columns[0].shape
    total = jnp.zeros((rows, 1), jnp.float32)
    for column in columns:
        value = column[...].astype(jnp.float32)
        total = total + jnp.sum(value * value, axis=-1, keepdims=True)
    inverse = lax.rsqrt(total / (width * len(columns)) + norm_eps)
    for e, column in enumerate(columns):
        place = at(scalars[0] ^ e, width)
        value = column[...].astype(jnp.float32) * inverse * gain[:, place]
        normed[:, place] = value.astype(jnp.bfloat16)
        kept[:, place] = column[at(scalars[1], kept.shape[0]), :]


def up_kernel(scalars, scale, *refs, n, reps):
    normed, pieces, (hidden, weight) = refs[:n], refs[n:-2], refs[-2:]
    rows = normed[0].shape[0]
    own, pieces = pieces[0], pieces[1:]
    depth = own.shape[0]
    weight[at(scalars[0], depth), :] = own[...]
    for place, piece in enumerate(pieces):
        d, k = place // reps + 1, place % reps
        part = lax.rem(scalars[1] - k + reps, reps)
        weight[at((scalars[0] ^ d) * reps + part, depth // reps), :] = piece[...]
    for d in range(n):
        value = jnp.dot(normed[d][...], weight[...], preferred_element_type=jnp.float32)
        value = jnp.maximum(value * scale[...], 0.0)
        hidden[d * rows : (d + 1) * rows, :] = (value * value).astype(jnp.bfloat16)


def down_kernel(scalars, hidden, scale, *refs, n):
    *pieces, stays, goes, weight = refs
    size = weight.shape[0] // len(pieces)
    for k, piece in enumerate(pieces):
        part = lax.rem(scalars[0] - k + len(pieces), len(pieces))
        weight[at(part, size), :] = piece[...]
    half = stays.shape[0] // n
    for b in range(n):
        for out, side in ((goes, 1 - scalars[1]), (stays, scalars[1])):
            value = jnp.dot(
                hidden[at(2 * b + side, half), :], weight[...], preferred_element_type=jnp.float32
            )
            out[b * half : (b + 1) * half, :] = (value * scale[...]).astype(jnp.bfloat16)


def fold_kernel(scalars, stayed, got, stays, goes, *, n):
    half = stays.shape[0] // n
    for b in range(n):
        for out, side in ((goes, 1 - scalars[0]), (stays, scalars[0])):
            place = at(2 * b + side, half)
            value = stayed[place, :].astype(jnp.float32) + got[place, :].astype(jnp.float32)
            out[b * half : (b + 1) * half, :] = value.astype(jnp.bfloat16)


def sum_kernel(scalars, *refs, n):
    del scalars
    pairs, outs = refs[:-n], refs[-n:]
    rows, width = outs[0].shape[0], pairs[0].shape[1]
    for c in range(len(pairs) // 2):
        stayed, got = pairs[2 * c], pairs[2 * c + 1]
        for e, out in enumerate(outs):
            here = slice(e * rows, (e + 1) * rows)
            value = stayed[here, :].astype(jnp.float32) + got[here, :].astype(jnp.float32)
            out[:, c * width : (c + 1) * width] = value.astype(jnp.bfloat16)


def final_kernel(scalars, kept, *refs, n):
    *sums, out = refs
    width = out.shape[1] // n
    groups = len(sums) // n
    for q in range(n):
        place = at(scalars[0] ^ q, width)
        value = kept[:, place].astype(jnp.float32)
        for e in range(n):
            side, column = divmod(q ^ e, n // groups)
            piece = sums[side * n + e][:, column * width : (column + 1) * width]
            value = value + piece.astype(jnp.float32)
        out[:, place] = value.astype(jnp.bfloat16)


def place_kernel(scalars, *refs):
    *parts, out = refs
    for e, part in enumerate(parts):
        out[at(scalars[e], part.shape[0]), :] = part[...]


def exchange_body(sizes):
    reps, n, m = sizes["rep"], sizes["fs"], sizes["tp"]
    axes = ("rep", "fs", "tp")
    tp_bits = bits_of(m)

    def hop(values, rep=0, fs=0, tp=0):
        pairs = []
        for a in range(reps):
            for b in range(n):
                for c in range(m):
                    target = (((a + rep) % reps) * n + (b ^ fs)) * m + (c ^ tp)
                    pairs.append(((a * n + b) * m + c, target))
        return lax.ppermute(values, axes, pairs)

    def spread_fs(own):
        held = [own]
        for d in range(1, n):
            low = d & -d
            held.append(hop(held[d ^ low], fs=low))
        return held

    def gather_tp(own):
        held = {0: own}
        for bit in reversed(tp_bits):
            for e in list(held):
                held[e ^ bit] = hop(held[e], tp=bit)
        return [held[e] for e in range(m)]

    def rank_of_rows(j):
        place = 0
        for bit in tp_bits:
            place = 2 * place + (j // bit) % 2
        return place

    def body(
        tokens,
        mix_gain,
        group_weight,
        group_scale,
        mlp_gain,
        up_weight,
        up_scale,
        down_weight,
        down_scale,
    ):
        rows, model_width = tokens.shape
        r, i, j = (lax.axis_index(axis) for axis in axes)
        width = group_weight.shape[1]
        units = up_weight.shape[1] // n
        cols = down_weight.shape[1]

        mixer = spread_fs(group_weight.astype(jnp.bfloat16))
        (packed,) = local(prep_kernel, [array((rows + 16, width))], [j], tokens)
        blocks = spread_fs(packed)

        def send_parts(block_of):
            got = [[block_of(0).astype(jnp.bfloat16)]]
            for d in range(1, n):
                block = block_of(d)
                part = block.shape[0] // reps
                part = lax.dynamic_slice_in_dim(block, r * part, part, 0).astype(jnp.bfloat16)
                part = hop(part, fs=d)
                got.append([part] + [hop(part, rep=k) for k in range(1, reps)])
            return got

        ups = send_parts(lambda d: lax.dynamic_slice_in_dim(up_weight, (i ^ d) * units, units, 1))
        downs = send_parts(lambda d: lax.dynamic_slice_in_dim(down_weight, (i ^ d) * units, units, 0))

        gain = lax.dynamic_slice_in_dim(mix_gain.reshape(1, -1), j * width, width, 1)
        normed, kept = [], None
        part_rows = rows // m
        for d in range(n):
            (carried,) = local(
                mix_kernel, [array((rows, width))], [i, j],
                blocks[d], gain, group_scale, *mixer,
                scratch=[((n * group_weight.shape[0], width), jnp.bfloat16)],
                flops=2 * rows * width * (width + LENGTH),
            )
            columns = gather_tp(carried)
            value, part = local(
                norm_kernel, [array((rows, model_width)), array((part_rows, model_width))],
                [j, rank_of_rows(j)], mlp_gain.reshape(1, -1), *columns,
                flops=10 * rows * model_width,
            )
            normed.append(value)
            kept = part if d == 0 else kept
        (hidden,) = local(
            functools.partial(up_kernel, n=n, reps=reps), [array((n * rows, units))], [i, r],
            lax.dynamic_slice_in_dim(up_scale, i * units, units, 1),
            *normed, *(p for block in ups for p in block),
            scratch=[((model_width, units), jnp.bfloat16)],
            flops=2 * n * rows * model_width * units,
        )

        sums = []
        for d in range(n):
            scale = lax.dynamic_slice_in_dim(down_scale, (i ^ d) * cols, cols, 1)
            half = array((n * rows // 2, cols))
            stays, goes = local(
                functools.partial(down_kernel, n=n), [half, half], [r, j % 2],
                hidden, scale, *downs[d],
                scratch=[((units, cols), jnp.bfloat16)],
                flops=2 * n * rows * units * cols,
            )
            for bit in tp_bits[1:]:
                got = hop(goes, tp=bit // 2)
                half = array((half.shape[0] // 2, cols))
                stays, goes = local(
                    functools.partial(fold_kernel, n=n), [half, half],
                    [(j // bit) % 2], stays, got,
                )
            sums += [stays, hop(goes, tp=tp_bits[-1])]
        terms = []
        for side in range(2):
            mine = sums[side * n : (side + 1) * n]
            outs = local(
                functools.partial(sum_kernel, n=n),
                [array((part_rows, cols * n // 2))] * n, [i], *mine,
            )
            terms += [outs[0]] + [hop(outs[e], fs=e) for e in range(1, n)]
        (out,) = local(
            functools.partial(final_kernel, n=n), [array((part_rows, model_width))], [i],
            kept, *terms,
        )
        parts = gather_tp(out)
        (out,) = local(
            place_kernel, [array((rows, model_width))],
            [rank_of_rows(j ^ e) for e in range(m)], *parts,
        )
        return out

    return body


def solution(mesh):
    in_specs = (
        P(("rep", "fs"), None),
        P(),
        P("fs", "tp"),
        P(None, "tp"),
        P(),
        P("fs", "tp"),
        P(None, "tp"),
        P("tp", "fs"),
        P(),
    )
    out_specs = P(("rep", "fs"), None)
    sizes = dict(mesh.shape)

    def layer(*args):
        tokens, up = args[0], args[5]
        moved = up.size // sizes["tp"]
        gathered = tokens.size // sizes["rep"]
        powers = all(sizes[a] & (sizes[a] - 1) == 0 for a in ("fs", "tp"))
        fits = sizes["tp"] == sizes["fs"] == GROUPS
        chosen = exchange_body(sizes) if powers and fits and gathered < moved else gather_body
        return jax.shard_map(
            chosen, mesh=mesh, in_specs=in_specs, out_specs=out_specs, check_vma=False
        )(*args)

    return layer
```

```python
import functools
import math

import jax
import jax.numpy as jnp
from jax import lax
from jax.experimental import pallas as pl
from jax.experimental.pallas import tpu as pltpu
from jax.sharding import PartitionSpec as P


GROUPS = 4
LENGTH = 128


norm_eps = 1e-06


def norm_rows(values, gain):
    promoted = values.astype(jnp.float32)
    inverse = lax.rsqrt(jnp.mean(promoted * promoted, axis=-1, keepdims=True) + norm_eps)
    return (promoted * inverse * gain).astype(jnp.bfloat16)


def band_means(inputs, window, seq_length):
    row_count, columns = inputs.shape
    by_sequence = inputs.reshape(row_count // seq_length, seq_length, columns)
    position = jnp.arange(seq_length, dtype=jnp.int32)
    offset = position[:, None] - position[None, :]
    band_mask = ((offset >= 0) & (offset < window)).astype(jnp.bfloat16)
    divisor = jnp.minimum(position + 1, window).astype(jnp.float32)
    summed = jnp.einsum("ts,nsc->ntc", band_mask, by_sequence, preferred_element_type=jnp.float32)
    return (summed / divisor[None, :, None] - by_sequence.astype(jnp.float32)).reshape(
        row_count, columns
    )


def gather_body(
    tokens,
    mix_gain,
    group_weight,
    group_scale,
    mlp_gain,
    up_weight,
    up_scale,
    down_weight,
    down_scale,
):
    model_width = tokens.shape[1]
    group_width = model_width // GROUPS
    own_cols = group_weight.shape[1]
    column_start = lax.axis_index("tp") * own_cols
    group_index = column_start // group_width
    normed = norm_rows(tokens, mix_gain)
    inputs = lax.dynamic_slice_in_dim(normed, group_index * group_width, group_width, 1)
    window = jnp.left_shift(jnp.int32(2), group_index)
    pooled = band_means(inputs, window, LENGTH).astype(jnp.bfloat16)
    mixed_cols = (
        jnp.dot(
            pooled,
            lax.all_gather(group_weight.astype(jnp.bfloat16), "fs", axis=0, tiled=True),
            preferred_element_type=jnp.float32,
        )
        * group_scale
    )
    own_tokens = lax.dynamic_slice_in_dim(tokens, column_start, own_cols, 1)
    carried_cols = (own_tokens.astype(jnp.float32) + mixed_cols).astype(jnp.bfloat16)
    carried = lax.all_gather(carried_cols, "tp", axis=1, tiled=True)
    normed_mlp = norm_rows(carried, mlp_gain)
    pre_act = (
        jnp.dot(
            normed_mlp,
            lax.all_gather(up_weight.astype(jnp.bfloat16), "fs", axis=0, tiled=True),
            preferred_element_type=jnp.float32,
        )
        * up_scale
    )
    hidden = jnp.square(jax.nn.relu(pre_act)).astype(jnp.bfloat16)
    partial_value = (
        jnp.dot(
            hidden,
            lax.all_gather(down_weight.astype(jnp.bfloat16), "fs", axis=1, tiled=True),
            preferred_element_type=jnp.float32,
        )
        * down_scale
    )
    summed = lax.psum(partial_value.astype(jnp.bfloat16), "tp").astype(jnp.float32)
    return (carried.astype(jnp.float32) + summed).astype(jnp.bfloat16)


def bits_of(count):
    return [1 << b for b in range(count.bit_length() - 1)]


def local(kernel, outs, scalars, *arrays, scratch=(), flops=0):
    moved = sum(a.size * a.dtype.itemsize for a in (*arrays, *outs))
    held = moved + sum(math.prod(shape) * jnp.dtype(kind).itemsize for shape, kind in scratch)
    return pl.pallas_call(
        kernel,
        out_shape=outs,
        in_specs=[pl.BlockSpec(memory_space=pltpu.SMEM)]
        + [pl.BlockSpec(memory_space=pltpu.VMEM)] * len(arrays),
        out_specs=[pl.BlockSpec(memory_space=pltpu.VMEM)] * len(outs),
        scratch_shapes=[pltpu.VMEM(shape, kind) for shape, kind in scratch],
        compiler_params=pltpu.CompilerParams(vmem_limit_bytes=min(3 * held + (8 << 20), 60 << 20)),
        cost_estimate=pl.CostEstimate(flops=max(flops, 1 << 20), bytes_accessed=moved, transcendentals=0),
    )(scalars, *arrays)


def array(shape, kind=jnp.bfloat16):
    return jax.ShapeDtypeStruct(shape, kind)


def at(index, size):
    return pl.ds(pl.multiple_of(index * size, size), size)


def rows_of(j, m):
    place = 0
    for bit in bits_of(m):
        place = 2 * place + (j // bit) % 2
    return place


def prep_kernel(scalars, tokens, packed):
    rows, width = tokens.shape[0], packed.shape[1]
    promoted = tokens[...].astype(jnp.float32)
    inverse = lax.rsqrt(jnp.mean(promoted * promoted, axis=-1, keepdims=True) + norm_eps)
    lane = lax.broadcasted_iota(jnp.int32, (rows, 128), 1)
    pieces = jnp.zeros((rows, 128), jnp.float32)
    for place in range(3):
        piece = inverse.astype(jnp.bfloat16).astype(jnp.float32)
        pieces = jnp.where(lane == place, piece, pieces)
        inverse = inverse - piece
    packed[:rows, :] = tokens[:, at(scalars[2], width)]
    packed[rows:, :] = jnp.zeros((packed.shape[0] - rows, width), jnp.bfloat16)
    packed[rows:, :rows] = jnp.transpose(pieces)[: packed.shape[0] - rows].astype(jnp.bfloat16)


def columns_kernel(scalars, weight, own, *outs):
    rows, units = outs[0].shape
    own[...] = weight[:, at(scalars[1], units)].astype(jnp.bfloat16)
    for d, out in enumerate(outs, 1):
        out[...] = weight[at(scalars[0], rows), at(scalars[1] ^ d, units)].astype(jnp.bfloat16)


def rows_kernel(scalars, weight, own, *outs):
    rows, units = outs[0].shape[0], own.shape[0]
    own[...] = weight[at(scalars[1], units), :].astype(jnp.bfloat16)
    for d, out in enumerate(outs, 1):
        part = (scalars[1] ^ d) * (units // rows) + scalars[0]
        out[...] = weight[at(part, rows), :].astype(jnp.bfloat16)


def mix_kernel(scalars, packed, gain, scale, *refs):
    *pieces, carried, mixer = refs
    (rows, width), depth = carried.shape, pieces[0].shape[0]
    for d, piece in enumerate(pieces):
        mixer[at(scalars[1] ^ d, depth), :] = piece[...]
    tokens = packed[:rows, :].astype(jnp.float32)
    three = packed[rows:, :rows].astype(jnp.float32)
    inverse = three[0:1] + three[1:2] + three[2:3]
    inverse = jnp.transpose(jnp.broadcast_to(inverse, (128, rows)))[:, :1]
    normed = (tokens * inverse * gain[:, at(scalars[2], width)]).astype(jnp.bfloat16)
    window = jnp.left_shift(jnp.int32(2), scalars[2])
    row = lax.broadcasted_iota(jnp.int32, (LENGTH, LENGTH), 0)
    offset = row - lax.broadcasted_iota(jnp.int32, (LENGTH, LENGTH), 1)
    band = jnp.where((offset >= 0) & (offset < window), 1.0, 0.0).astype(jnp.bfloat16)
    position = lax.broadcasted_iota(jnp.int32, (LENGTH, 1), 0)
    divisor = jnp.minimum(position + 1, window).astype(jnp.float32)
    for first in range(0, rows, LENGTH):
        here = slice(first, first + LENGTH)
        summed = jnp.dot(band, normed[here], preferred_element_type=jnp.float32)
        pooled = (summed / divisor - normed[here].astype(jnp.float32)).astype(jnp.bfloat16)
        mixed = jnp.dot(pooled, mixer[...], preferred_element_type=jnp.float32) * scale[...]
        carried[here, :] = (tokens[here] + mixed).astype(jnp.bfloat16)


def up_kernel(scalars, gain, scale, *refs, n, m, reps):
    columns, pieces, (hidden, weight, values) = refs[: n * m], refs[n * m : -3], refs[-3:]
    rows, width = columns[0].shape
    units = weight.shape[1]

    def put(piece, block, part, parts):
        size = width // parts
        place = block * parts + part
        tall = jnp.transpose(jnp.broadcast_to(gain[:, at(place, size)], (128, size)))[:, :1]
        weight[at(place, size), :] = (piece[...].astype(jnp.float32) * tall).astype(jnp.bfloat16)

    put(pieces[0], scalars[1], 0, 1)
    for place, piece in enumerate(pieces[1:]):
        d, k = place // reps + 1, place % reps
        put(piece, scalars[1] ^ d, lax.rem(scalars[0] - k + reps, reps), reps)
    for b in range(n):
        total = jnp.zeros((rows, 1), jnp.float32)
        for e in range(m):
            column = columns[b * m + e][...]
            values[:, at(scalars[2] ^ e, width)] = column
            column = column.astype(jnp.float32)
            total = total + jnp.sum(column * column, axis=-1, keepdims=True)
        inverse = lax.rsqrt(total / (width * m) + norm_eps)
        own_scale = scale[:, at(scalars[1], units)]
        value = jnp.dot(values[...], weight[...], preferred_element_type=jnp.float32)
        value = jnp.maximum(value * inverse * own_scale, 0.0)
        hidden[b * rows : (b + 1) * rows, :] = (value * value).astype(jnp.bfloat16)


def down_kernel(scalars, hidden, scale, *refs, n, d):
    *pieces, stays, goes, weight = refs
    size = weight.shape[0] // len(pieces)
    for k, piece in enumerate(pieces):
        part = lax.rem(scalars[0] - k + len(pieces), len(pieces))
        weight[at(part, size), :] = piece[...]
    half, cols = stays.shape[0] // n, stays.shape[1]
    mine = scalars[2] % 2
    own_scale = scale[:, at(scalars[1] ^ d, cols)]
    for out, side in ((goes, 1 - mine), (stays, mine)):
        for b in range(n):
            value = jnp.dot(
                hidden[at(2 * b + side, half), :], weight[...], preferred_element_type=jnp.float32
            )
            out[b * half : (b + 1) * half, :] = (value * own_scale).astype(jnp.bfloat16)


def fold_kernel(scalars, stayed, got, stays, goes, *, n, bit):
    half = stays.shape[0] // n
    mine = (scalars[2] // bit) % 2
    for b in range(n):
        for out, side in ((goes, 1 - mine), (stays, mine)):
            place = at(2 * b + side, half)
            value = stayed[place, :].astype(jnp.float32) + got[place, :].astype(jnp.float32)
            out[b * half : (b + 1) * half, :] = value.astype(jnp.bfloat16)


def sum_kernel(scalars, *refs, n):
    del scalars
    pairs, outs = refs[:-n], refs[-n:]
    rows, width = outs[0].shape[0], pairs[0].shape[1]
    for c in range(len(pairs) // 2):
        stayed, got = pairs[2 * c], pairs[2 * c + 1]
        for e, out in enumerate(outs):
            here = slice(e * rows, (e + 1) * rows)
            value = stayed[here, :].astype(jnp.float32) + got[here, :].astype(jnp.float32)
            out[:, c * width : (c + 1) * width] = value.astype(jnp.bfloat16)


def final_kernel(scalars, *refs, n, m, groups):
    columns, terms, out = refs[:m], refs[m:-1], refs[-1]
    rows, width = out.shape[0], columns[0].shape[1]
    here = at(rows_of(scalars[2], m), rows)
    for q in range(n):
        value = jnp.zeros((rows, width), jnp.float32)
        for e in range(n):
            for g, group in enumerate(groups):
                if q ^ e in group:
                    place = group.index(q ^ e) * width
                    piece = terms[g * n + e][:, place : place + width]
                    value = value + piece.astype(jnp.float32)
        out[:, at(scalars[1] ^ q, width)] = value.astype(jnp.bfloat16)
    for e in range(m):
        place = at(scalars[2] ^ e, width)
        value = columns[e][here, :].astype(jnp.float32) + out[:, place].astype(jnp.float32)
        out[:, place] = value.astype(jnp.bfloat16)


def place_kernel(scalars, *refs, m):
    *parts, out = refs
    for e, part in enumerate(parts):
        out[at(rows_of(scalars[2] ^ e, m), part.shape[0]), :] = part[...]


def exchange_body(sizes):
    reps, n, m = sizes["rep"], sizes["fs"], sizes["tp"]
    axes = ("rep", "fs", "tp")
    tp_bits = bits_of(m)

    def hop(values, rep=0, fs=0, tp=0):
        pairs = []
        for a in range(reps):
            for b in range(n):
                for c in range(m):
                    target = (((a + rep) % reps) * n + (b ^ fs)) * m + (c ^ tp)
                    pairs.append(((a * n + b) * m + c, target))
        return lax.ppermute(values, axes, pairs)

    def spread_fs(own):
        held = [own]
        for d in range(1, n):
            low = d & -d
            held.append(hop(held[d ^ low], fs=low))
        return held

    def gather_tp(own):
        held = {0: own}
        for bit in reversed(tp_bits):
            for e in list(held):
                held[e ^ bit] = hop(held[e], tp=bit)
        return [held[e] for e in range(m)]

    def body(
        tokens,
        mix_gain,
        group_weight,
        group_scale,
        mlp_gain,
        up_weight,
        up_scale,
        down_weight,
        down_scale,
    ):
        rows, model_width = tokens.shape
        me = jnp.stack([lax.axis_index(axis) for axis in axes])
        width = group_weight.shape[1]
        units = up_weight.shape[1] // n
        cols = down_weight.shape[1]
        part_rows = rows // m

        mixer = spread_fs(group_weight.astype(jnp.bfloat16))
        (packed,) = local(prep_kernel, [array((rows + 16, width))], me, tokens)
        blocks = spread_fs(packed)

        def send_parts(kernel, weight, own, part):
            own, *outs = local(kernel, [array(own)] + [array(part)] * (n - 1), me, weight)
            got = [own]
            for d, out in enumerate(outs, 1):
                out = hop(out, fs=d)
                got.append(out)
                got += [hop(out, rep=k) for k in range(1, reps)]
            return got

        ups = send_parts(columns_kernel, up_weight, (width, units), (width // reps, units))
        downs = send_parts(rows_kernel, down_weight, (units, cols), (units // reps, cols))

        columns = []
        for d in range(n):
            (carried,) = local(
                mix_kernel, [array((rows, width))], me,
                blocks[d], mix_gain.reshape(1, -1), group_scale, *mixer,
                scratch=[((n * group_weight.shape[0], width), jnp.bfloat16)],
                flops=2 * rows * width * (width + LENGTH),
            )
            columns += gather_tp(carried)
        (hidden,) = local(
            functools.partial(up_kernel, n=n, m=m, reps=reps), [array((n * rows, units))], me,
            mlp_gain.reshape(1, -1), up_scale, *columns, *ups,
            scratch=[((model_width, units), jnp.bfloat16), ((rows, model_width), jnp.bfloat16)],
            flops=2 * n * rows * model_width * units,
        )

        sums = []
        for d in range(n):
            half = array((n * rows // 2, cols))
            pieces = downs[:1] if d == 0 else downs[1 + (d - 1) * reps : 1 + d * reps]
            stays, goes = local(
                functools.partial(down_kernel, n=n, d=d), [half, half], me,
                hidden, down_scale, *pieces,
                scratch=[((units, cols), jnp.bfloat16)],
                flops=2 * n * rows * units * cols,
            )
            for bit in tp_bits[1:]:
                got = hop(goes, tp=bit // 2)
                half = array((half.shape[0] // 2, cols))
                stays, goes = local(
                    functools.partial(fold_kernel, n=n, bit=bit), [half, half],
                    me, stays, got,
                )
            sums.append((stays, hop(goes, tp=tp_bits[-1])))
        groups = [[*range(n // 2)]] + [[d] for d in range(n // 2, n)]
        terms = []
        for group in groups:
            outs = local(
                functools.partial(sum_kernel, n=n),
                [array((part_rows, cols * len(group)))] * n, me,
                *(term for d in group for term in sums[d]),
            )
            terms += [outs[0]]
            terms += [hop(outs[e], fs=e) for e in range(1, n)]
        (out,) = local(
            functools.partial(final_kernel, n=n, m=m, groups=groups),
            [array((part_rows, model_width))], me, *columns[:m], *terms,
        )
        (out,) = local(
            functools.partial(place_kernel, m=m), [array((rows, model_width))], me,
            *gather_tp(out),
        )
        return out

    return body


def solution(mesh):
    in_specs = (
        P(("rep", "fs"), None),
        P(),
        P("fs", "tp"),
        P(None, "tp"),
        P(),
        P("fs", "tp"),
        P(None, "tp"),
        P("tp", "fs"),
        P(),
    )
    out_specs = P(("rep", "fs"), None)
    sizes = dict(mesh.shape)

    def layer(*args):
        tokens, up = args[0], args[5]
        moved = up.size // sizes["tp"]
        gathered = tokens.size // sizes["rep"]
        powers = all(sizes[a] & (sizes[a] - 1) == 0 for a in ("fs", "tp"))
        fits = sizes["tp"] == sizes["fs"] == GROUPS
        chosen = exchange_body(sizes) if powers and fits and gathered < moved else gather_body
        return jax.shard_map(
            chosen, mesh=mesh, in_specs=in_specs, out_specs=out_specs, check_vma=False
        )(*args)

    return layer
```

```python
import functools
import math

import jax
import jax.numpy as jnp
from jax import lax
from jax.experimental import pallas as pl
from jax.experimental.pallas import tpu as pltpu
from jax.sharding import PartitionSpec as P


GROUPS = 4
LENGTH = 128


norm_eps = 1e-06


def norm_rows(values, gain):
    promoted = values.astype(jnp.float32)
    inverse = lax.rsqrt(jnp.mean(promoted * promoted, axis=-1, keepdims=True) + norm_eps)
    return (promoted * inverse * gain).astype(jnp.bfloat16)


def band_means(inputs, window, seq_length):
    row_count, columns = inputs.shape
    by_sequence = inputs.reshape(row_count // seq_length, seq_length, columns)
    position = jnp.arange(seq_length, dtype=jnp.int32)
    offset = position[:, None] - position[None, :]
    band_mask = ((offset >= 0) & (offset < window)).astype(jnp.bfloat16)
    divisor = jnp.minimum(position + 1, window).astype(jnp.float32)
    summed = jnp.einsum("ts,nsc->ntc", band_mask, by_sequence, preferred_element_type=jnp.float32)
    return (summed / divisor[None, :, None] - by_sequence.astype(jnp.float32)).reshape(
        row_count, columns
    )


def gather_body(
    tokens,
    mix_gain,
    group_weight,
    group_scale,
    mlp_gain,
    up_weight,
    up_scale,
    down_weight,
    down_scale,
):
    model_width = tokens.shape[1]
    group_width = model_width // GROUPS
    own_cols = group_weight.shape[1]
    column_start = lax.axis_index("tp") * own_cols
    group_index = column_start // group_width
    normed = norm_rows(tokens, mix_gain)
    inputs = lax.dynamic_slice_in_dim(normed, group_index * group_width, group_width, 1)
    window = jnp.left_shift(jnp.int32(2), group_index)
    pooled = band_means(inputs, window, LENGTH).astype(jnp.bfloat16)
    mixed_cols = (
        jnp.dot(
            pooled,
            lax.all_gather(group_weight.astype(jnp.bfloat16), "fs", axis=0, tiled=True),
            preferred_element_type=jnp.float32,
        )
        * group_scale
    )
    own_tokens = lax.dynamic_slice_in_dim(tokens, column_start, own_cols, 1)
    carried_cols = (own_tokens.astype(jnp.float32) + mixed_cols).astype(jnp.bfloat16)
    carried = lax.all_gather(carried_cols, "tp", axis=1, tiled=True)
    normed_mlp = norm_rows(carried, mlp_gain)
    pre_act = (
        jnp.dot(
            normed_mlp,
            lax.all_gather(up_weight.astype(jnp.bfloat16), "fs", axis=0, tiled=True),
            preferred_element_type=jnp.float32,
        )
        * up_scale
    )
    hidden = jnp.square(jax.nn.relu(pre_act)).astype(jnp.bfloat16)
    partial_value = (
        jnp.dot(
            hidden,
            lax.all_gather(down_weight.astype(jnp.bfloat16), "fs", axis=1, tiled=True),
            preferred_element_type=jnp.float32,
        )
        * down_scale
    )
    summed = lax.psum(partial_value.astype(jnp.bfloat16), "tp").astype(jnp.float32)
    return (carried.astype(jnp.float32) + summed).astype(jnp.bfloat16)


def bits_of(count):
    return [1 << b for b in range(count.bit_length() - 1)]


def local(kernel, outs, scalars, *arrays, scratch=(), flops=0):
    moved = sum(a.size * a.dtype.itemsize for a in (*arrays, *outs))
    held = moved + sum(math.prod(shape) * jnp.dtype(kind).itemsize for shape, kind in scratch)
    return pl.pallas_call(
        kernel,
        out_shape=outs,
        in_specs=[pl.BlockSpec(memory_space=pltpu.SMEM)]
        + [pl.BlockSpec(memory_space=pltpu.VMEM)] * len(arrays),
        out_specs=[pl.BlockSpec(memory_space=pltpu.VMEM)] * len(outs),
        scratch_shapes=[pltpu.VMEM(shape, kind) for shape, kind in scratch],
        compiler_params=pltpu.CompilerParams(vmem_limit_bytes=min(3 * held + (8 << 20), 60 << 20)),
        cost_estimate=pl.CostEstimate(flops=max(flops, 1 << 20), bytes_accessed=moved, transcendentals=0),
    )(scalars, *arrays)


def array(shape, kind=jnp.bfloat16):
    return jax.ShapeDtypeStruct(shape, kind)


def at(index, size):
    return pl.ds(pl.multiple_of(index * size, size), size)


def rows_of(j, m):
    place = 0
    for bit in bits_of(m):
        place = 2 * place + (j // bit) % 2
    return place


def prep_kernel(scalars, tokens, packed):
    rows, width = tokens.shape[0], packed.shape[1]
    promoted = tokens[...].astype(jnp.float32)
    inverse = lax.rsqrt(jnp.mean(promoted * promoted, axis=-1, keepdims=True) + norm_eps)
    lane = lax.broadcasted_iota(jnp.int32, (rows, 128), 1)
    pieces = jnp.zeros((rows, 128), jnp.float32)
    for place in range(3):
        piece = inverse.astype(jnp.bfloat16).astype(jnp.float32)
        pieces = jnp.where(lane == place, piece, pieces)
        inverse = inverse - piece
    packed[:rows, :] = tokens[:, at(scalars[2], width)]
    packed[rows:, :] = jnp.zeros((packed.shape[0] - rows, width), jnp.bfloat16)
    packed[rows:, :rows] = jnp.transpose(pieces)[: packed.shape[0] - rows].astype(jnp.bfloat16)


def columns_kernel(scalars, weight, own, *outs):
    rows, units = outs[0].shape
    own[...] = weight[:, at(scalars[1], units)].astype(jnp.bfloat16)
    for d, out in enumerate(outs, 1):
        out[...] = weight[at(scalars[0], rows), at(scalars[1] ^ d, units)].astype(jnp.bfloat16)


def rows_kernel(scalars, weight, own, *outs):
    rows, units = outs[0].shape[0], own.shape[0]
    own[...] = weight[at(scalars[1], units), :].astype(jnp.bfloat16)
    for d, out in enumerate(outs, 1):
        part = (scalars[1] ^ d) * (units // rows) + scalars[0]
        out[...] = weight[at(part, rows), :].astype(jnp.bfloat16)


def mix_kernel(scalars, packed, gain, scale, *refs):
    *pieces, carried, mixer = refs
    (rows, width), depth = carried.shape, pieces[0].shape[0]
    for d, piece in enumerate(pieces):
        mixer[at(scalars[1] ^ d, depth), :] = piece[...]
    tokens = packed[:rows, :].astype(jnp.float32)
    three = packed[rows:, :rows].astype(jnp.float32)
    inverse = three[0:1] + three[1:2] + three[2:3]
    inverse = jnp.transpose(jnp.broadcast_to(inverse, (128, rows)))[:, :1]
    normed = (tokens * inverse * gain[:, at(scalars[2], width)]).astype(jnp.bfloat16)
    window = jnp.left_shift(jnp.int32(2), scalars[2])
    row = lax.broadcasted_iota(jnp.int32, (LENGTH, LENGTH), 0)
    offset = row - lax.broadcasted_iota(jnp.int32, (LENGTH, LENGTH), 1)
    band = jnp.where((offset >= 0) & (offset < window), 1.0, 0.0).astype(jnp.bfloat16)
    position = lax.broadcasted_iota(jnp.int32, (LENGTH, 1), 0)
    divisor = jnp.minimum(position + 1, window).astype(jnp.float32)
    for first in range(0, rows, LENGTH):
        here = slice(first, first + LENGTH)
        summed = jnp.dot(band, normed[here], preferred_element_type=jnp.float32)
        pooled = (summed / divisor - normed[here].astype(jnp.float32)).astype(jnp.bfloat16)
        mixed = jnp.dot(pooled, mixer[...], preferred_element_type=jnp.float32) * scale[...]
        carried[here, :] = (tokens[here] + mixed).astype(jnp.bfloat16)


def scaled(piece, gain, place):
    size = piece.shape[0]
    tall = jnp.transpose(jnp.broadcast_to(gain[:, at(place, size)], (128, size)))[:, :1]
    return (piece[...].astype(jnp.float32) * tall).astype(jnp.bfloat16)


def gathered(columns, values, j):
    rows, width = columns[0].shape
    total = jnp.zeros((rows, 1), jnp.float32)
    for e, column in enumerate(columns):
        column = column[...]
        values[:, at(j ^ e, width)] = column
        column = column.astype(jnp.float32)
        total = total + jnp.sum(column * column, axis=-1, keepdims=True)
    return lax.rsqrt(total / (width * len(columns)) + norm_eps)


def part_of(scalars, place, reps):
    d, k = place // reps + 1, place % reps
    return (scalars[1] ^ d) * reps + lax.rem(scalars[0] - k + reps, reps)


def early_kernel(scalars, gain, *refs, blocks, m, reps):
    columns, pieces = refs[: blocks * m], refs[blocks * m : -5]
    weight, sums, inverses, missing, values = refs[-5:]
    rows, width = columns[0].shape
    weight[at(scalars[1], width), :] = scaled(pieces[0], gain, scalars[1])
    for place, piece in enumerate(pieces[1:]):
        part = part_of(scalars, place, reps)
        weight[at(part, width // reps), :] = scaled(piece, gain, part)
    last = at(part_of(scalars, len(pieces) - 1, reps), width // reps)
    weight[last, :] = jnp.zeros((width // reps, weight.shape[1]), jnp.bfloat16)
    for b in range(blocks):
        here = slice(b * rows, (b + 1) * rows)
        inverses[here, :] = gathered(columns[b * m : (b + 1) * m], values.at[b], scalars[2])
        missing[here, :] = values[b, :, last]
        sums[here, :] = jnp.dot(values[b], weight[...], preferred_element_type=jnp.float32)


def up_kernel(scalars, gain, scale, *refs, m, reps, last):
    columns, (piece, weight, sums, inverses, missing, hidden, values) = refs[:m], refs[m:]
    rows, units = columns[0].shape[0], weight.shape[1]
    own_scale = scale[:, at(scalars[1], units)]
    part = part_of(scalars, last, reps)
    piece = scaled(piece, gain, part)

    def put(b, value, inverse):
        value = jnp.maximum(value * inverse * own_scale, 0.0)
        hidden[b * rows : (b + 1) * rows, :] = (value * value).astype(jnp.bfloat16)

    blocks = sums.shape[0] // rows
    inverse = gathered(columns, values, scalars[2])
    for b in range(blocks):
        here = slice(b * rows, (b + 1) * rows)
        value = jnp.dot(missing[here, :], piece, preferred_element_type=jnp.float32)
        put(b, sums[here, :] + value, inverses[here, :])
    value = jnp.dot(values[...], weight[...], preferred_element_type=jnp.float32)
    rest = values[:, at(part, piece.shape[0])]
    put(blocks, value + jnp.dot(rest, piece, preferred_element_type=jnp.float32), inverse)


def down_kernel(scalars, hidden, scale, *refs, n, d):
    *pieces, stays, goes, weight = refs
    size = weight.shape[0] // len(pieces)
    for k, piece in enumerate(pieces):
        part = lax.rem(scalars[0] - k + len(pieces), len(pieces))
        weight[at(part, size), :] = piece[...]
    half, cols = stays.shape[0] // n, stays.shape[1]
    mine = scalars[2] % 2
    own_scale = scale[:, at(scalars[1] ^ d, cols)]
    for out, side in ((goes, 1 - mine), (stays, mine)):
        for b in range(n):
            value = jnp.dot(
                hidden[at(2 * b + side, half), :], weight[...], preferred_element_type=jnp.float32
            )
            out[b * half : (b + 1) * half, :] = (value * own_scale).astype(jnp.bfloat16)


def fold_kernel(scalars, stayed, got, stays, goes, *, n, bit):
    half = stays.shape[0] // n
    mine = (scalars[2] // bit) % 2
    for b in range(n):
        for out, side in ((goes, 1 - mine), (stays, mine)):
            place = at(2 * b + side, half)
            value = stayed[place, :].astype(jnp.float32) + got[place, :].astype(jnp.float32)
            out[b * half : (b + 1) * half, :] = value.astype(jnp.bfloat16)


def sum_kernel(scalars, *refs, n):
    del scalars
    pairs, outs = refs[:-n], refs[-n:]
    rows, width = outs[0].shape[0], pairs[0].shape[1]
    for c in range(len(pairs) // 2):
        stayed, got = pairs[2 * c], pairs[2 * c + 1]
        for e, out in enumerate(outs):
            here = slice(e * rows, (e + 1) * rows)
            value = stayed[here, :].astype(jnp.float32) + got[here, :].astype(jnp.float32)
            out[:, c * width : (c + 1) * width] = value.astype(jnp.bfloat16)


def pair_kernel(scalars, *refs, n):
    del scalars
    *pairs, own, relayed, goes = refs
    rows, width = own.shape[0], pairs[0].shape[1]
    for c in range(len(pairs) // 2):
        stayed, got = pairs[2 * c], pairs[2 * c + 1]
        there = slice(c * width, (c + 1) * width)
        for e in range(n):
            here = slice(e * rows, (e + 1) * rows)
            value = stayed[here, :].astype(jnp.float32) + got[here, :].astype(jnp.float32)
            value = value.astype(jnp.bfloat16)
            if e % 2:
                goes[e // 2 * rows : (e // 2 + 1) * rows, there] = value
            elif e:
                relayed[:, there] = value
            else:
                own[:, there] = value


def relay_kernel(scalars, mine, got, out):
    del scalars
    rows, width = out.shape[0], out.shape[1] // 2
    for c in range(2):
        here, there = slice(c * width, (c + 1) * width), slice((1 - c) * width, (2 - c) * width)
        value = mine[:, here].astype(jnp.float32) + got[rows:, there].astype(jnp.float32)
        out[:, here] = value.astype(jnp.bfloat16)


def final_kernel(scalars, *refs, n, m, groups):
    columns, (own, paired, crossed), terms, out = refs[:m], refs[m : m + 3], refs[m + 3 : -1], refs[-1]
    rows, width = out.shape[0], columns[0].shape[1]
    here = at(rows_of(scalars[2], m), rows)
    for q in range(n):
        place, other = slice(q % 2 * width, (q % 2 + 1) * width), slice((1 - q % 2) * width, (2 - q % 2) * width)
        if q < 2:
            value = own[:, place].astype(jnp.float32) + paired[:rows, other].astype(jnp.float32)
        else:
            value = crossed[:, place].astype(jnp.float32)
        for e in range(n):
            for g, group in enumerate(groups):
                if q ^ e == group:
                    value = value + terms[g * n + e][...].astype(jnp.float32)
        out[:, at(scalars[1] ^ q, width)] = value.astype(jnp.bfloat16)
    for e in range(m):
        place = at(scalars[2] ^ e, width)
        value = columns[e][here, :].astype(jnp.float32) + out[:, place].astype(jnp.float32)
        out[:, place] = value.astype(jnp.bfloat16)


def place_kernel(scalars, *refs, m):
    *parts, out = refs
    for e, part in enumerate(parts):
        out[at(rows_of(scalars[2] ^ e, m), part.shape[0]), :] = part[...]


def exchange_body(sizes):
    reps, n, m = sizes["rep"], sizes["fs"], sizes["tp"]
    axes = ("rep", "fs", "tp")
    tp_bits = bits_of(m)

    def hop(values, rep=0, fs=0, tp=0):
        pairs = []
        for a in range(reps):
            for b in range(n):
                for c in range(m):
                    target = (((a + rep) % reps) * n + (b ^ fs)) * m + (c ^ tp)
                    pairs.append(((a * n + b) * m + c, target))
        return lax.ppermute(values, axes, pairs)

    def spread_fs(own):
        held = [own]
        for d in range(1, n):
            low = d & -d
            held.append(hop(held[d ^ low], fs=low))
        return held

    def gather_tp(own):
        held = {0: own}
        for bit in reversed(tp_bits):
            for e in list(held):
                held[e ^ bit] = hop(held[e], tp=bit)
        return [held[e] for e in range(m)]

    def body(
        tokens,
        mix_gain,
        group_weight,
        group_scale,
        mlp_gain,
        up_weight,
        up_scale,
        down_weight,
        down_scale,
    ):
        rows, model_width = tokens.shape
        me = jnp.stack([lax.axis_index(axis) for axis in axes])
        width = group_weight.shape[1]
        units = up_weight.shape[1] // n
        cols = down_weight.shape[1]
        part_rows = rows // m

        mixer = spread_fs(group_weight.astype(jnp.bfloat16))
        (packed,) = local(prep_kernel, [array((rows + 8, width))], me, tokens)
        blocks = spread_fs(packed)

        def send_parts(kernel, weight, own, part):
            own, *outs = local(kernel, [array(own)] + [array(part)] * (n - 1), me, weight)
            got = [own]
            for d, out in enumerate(outs, 1):
                out = hop(out, fs=d)
                got.append(out)
                got += [hop(out, rep=k) for k in range(1, reps)]
            return got

        ups = send_parts(columns_kernel, up_weight, (width, units), (width // reps, units))
        downs = send_parts(rows_kernel, down_weight, (units, cols), (units // reps, cols))

        columns = []
        for d in range(n):
            (carried,) = local(
                mix_kernel, [array((rows, width))], me,
                blocks[d], mix_gain.reshape(1, -1), group_scale, *mixer,
                scratch=[((n * group_weight.shape[0], width), jnp.bfloat16)],
                flops=2 * rows * width * (width + LENGTH),
            )
            columns += gather_tp(carried)
        early = n - 1
        started = local(
            functools.partial(early_kernel, blocks=early, m=m, reps=reps),
            [
                array((model_width, units)),
                array((early * rows, units), jnp.float32),
                array((early * rows, 1), jnp.float32),
                array((early * rows, width // reps)),
            ],
            me, mlp_gain.reshape(1, -1), *columns[: early * m], *ups[:-1],
            scratch=[((early, rows, model_width), jnp.bfloat16)],
            flops=2 * early * rows * model_width * units,
        )
        (hidden,) = local(
            functools.partial(up_kernel, m=m, reps=reps, last=len(ups) - 2),
            [array((n * rows, units))], me,
            mlp_gain.reshape(1, -1), up_scale, *columns[early * m :], ups[-1], *started,
            scratch=[((rows, model_width), jnp.bfloat16)],
            flops=2 * rows * model_width * units,
        )

        sums = []
        for d in range(n):
            half = array((n * rows // 2, cols))
            pieces = downs[:1] if d == 0 else downs[1 + (d - 1) * reps : 1 + d * reps]
            stays, goes = local(
                functools.partial(down_kernel, n=n, d=d), [half, half], me,
                hidden, down_scale, *pieces,
                scratch=[((units, cols), jnp.bfloat16)],
                flops=2 * n * rows * units * cols,
            )
            for bit in tp_bits[1:]:
                got = hop(goes, tp=bit // 2)
                half = array((half.shape[0] // 2, cols))
                stays, goes = local(
                    functools.partial(fold_kernel, n=n, bit=bit), [half, half],
                    me, stays, got,
                )
            sums.append((stays, hop(goes, tp=tp_bits[-1])))
        half = array((part_rows, 2 * cols))
        own, relayed, goes = local(
            functools.partial(pair_kernel, n=n), [half, half, array((2 * part_rows, 2 * cols))],
            me, *sums[0], *sums[1],
        )
        paired = hop(goes, fs=1)
        (relayed,) = local(relay_kernel, [half], me, relayed, paired)
        terms = [own, paired, hop(relayed, fs=2)]
        groups = range(2, n)
        for d in groups:
            outs = local(functools.partial(sum_kernel, n=n), [array((part_rows, cols))] * n, me, *sums[d])
            terms += [outs[0]] + [hop(outs[e], fs=e) for e in range(1, n)]
        (out,) = local(
            functools.partial(final_kernel, n=n, m=m, groups=groups),
            [array((part_rows, model_width))], me, *columns[:m], *terms,
        )
        (out,) = local(
            functools.partial(place_kernel, m=m), [array((rows, model_width))], me,
            *gather_tp(out),
        )
        return out

    return body


def solution(mesh):
    in_specs = (
        P(("rep", "fs"), None),
        P(),
        P("fs", "tp"),
        P(None, "tp"),
        P(),
        P("fs", "tp"),
        P(None, "tp"),
        P("tp", "fs"),
        P(),
    )
    out_specs = P(("rep", "fs"), None)
    sizes = dict(mesh.shape)

    def layer(*args):
        tokens, up = args[0], args[5]
        moved = up.size // sizes["tp"]
        gathered = tokens.size // sizes["rep"]
        powers = all(sizes[a] & (sizes[a] - 1) == 0 for a in ("fs", "tp"))
        fits = sizes["tp"] == sizes["fs"] == GROUPS == 4
        chosen = exchange_body(sizes) if powers and fits and gathered < moved else gather_body
        return jax.shard_map(
            chosen, mesh=mesh, in_specs=in_specs, out_specs=out_specs, check_vma=False
        )(*args)

    return layer
```
